32 devices in a mesh: sp: 16 (over z, y, x), tp: 2 (over core).
Axes of the slice: x: 2, y: 2, z: 4, core: 2. Of those that a mesh axis runs over, the one named last changes fastest.
Arguments:
- normed: bfloat16 [4096, 2048], P(('sp', 'tp')), may hold values from -40 to 40
- query_weight: bfloat16 [2048, 2048], P(None, 'tp'), may hold values from -1.5 to 1.5
- key_weight: bfloat16 [2048, 2048], P(None, 'tp'), may hold values from -1 to 1
- value_weight: bfloat16 [2048, 2048], P(None, 'tp'), may hold values from -0.125 to 0.125
- pool_in_weight: bfloat16 [2048, 1024], P(None, 'tp'), may hold values from -0.125 to 0.125
- pool_weight: bfloat16 [8, 128, 128], P('tp'), may hold values from -0.5 to 0.5
- map_balance: float32 [8], replicated, may hold values from 0.3 to 0.8
- head_gain: float32 [256], replicated, may hold values from 0.1 to 1.9
- contrast_out_weight: bfloat16 [2048, 2048], P('tp'), may hold values from -0.109375 to 0.109375
- pool_out_weight: bfloat16 [1024, 2048], P('tp'), may hold values from -0.109375 to 0.109375
Outputs:
- layer_out: bfloat16 [4096, 2048], P(('sp', 'tp'))
The draws below stay inside these ranges and needn't reach their ends.
All inputs are finite; a program needn't handle non-finite values.
Results may differ from the reference program's by a relative error of at most 0.03.
Values may be sent and summed in bfloat16 or wider, within the bound.
A program may use at most 128 MiB of HBM per device.

```python
import math
import jax
import jax.numpy as jnp
from jax import lax

D = 2048
HEADS = 8
HEAD_DIM = 128
GROUPS = 8
GROUP_WIDTH = 128
TOKENS = 4096
N_TP = 2


def shared_keys(key):
    gaussian = jnp.clip(jax.random.normal(jax.random.fold_in(key, 11), (D, 2 * HEADS * HEAD_DIM), jnp.float32), -6.0, 6.0)
    return gaussian * (1.3 / math.sqrt(D))


def draw_key_weight(key, part):
    return shared_keys(key).astype(jnp.bfloat16)


def draw_query_weight(key, part):
    independent = jnp.clip(jax.random.normal(jax.random.fold_in(key, 12), (D, 2 * HEADS * HEAD_DIM), jnp.float32), -6.0, 6.0) * (1.3 / math.sqrt(D))
    aligned = independent
    return aligned.astype(jnp.bfloat16)


def draw_normed(key, part):
    gaussian = jax.random.normal(jax.random.fold_in(key, 21), (TOKENS, D), jnp.float32)
    return jnp.clip(gaussian, -6.0, 6.0).astype(jnp.bfloat16)


def level_of(own_key, dims, pieces, smallest, high):
    def one(dim, parts):
        heights = jax.random.uniform(jax.random.fold_in(jax.random.fold_in(own_key, 6), dim), (parts,), jnp.float32, smallest / len(pieces), high / len(pieces))
        return jnp.repeat(jnp.exp(heights), dims[dim] // parts).reshape((-1,) + (1,) * (len(dims) - dim - 1))

    gain = one(*pieces[0])
    for cut in pieces[1:]:
        gain = gain * one(*cut)
    return gain


def noise(own_key, dims, scale, most, shards=(), held_as=jnp.bfloat16):
    array = jax.random.normal(own_key, dims, jnp.float32) * scale
    if len(shards) > 0:
        array = level_of(own_key, dims, shards, -0.22, 0.18) * array
    return jnp.clip(array, min=-most, max=most).astype(held_as)


def setup_inputs(seed: int = 0) -> dict:
    streams_of = jax.random.split(jax.random.key(seed), 11)
    normed = draw_normed(jax.random.fold_in(streams_of[10], 71), 0)
    query_weight = draw_query_weight(jax.random.fold_in(streams_of[10], 71), 0)
    key_weight = draw_key_weight(jax.random.fold_in(streams_of[10], 71), 0)
    value_weight = noise(streams_of[3], (D, 2 * HEADS * HEAD_DIM), D ** -0.5, 0.125, ((1, 2),))
    pool_in_weight = noise(streams_of[4], (D, GROUPS * GROUP_WIDTH), D ** -0.5, 0.125, ((1, 2),))
    pool_weight = noise(streams_of[5], (GROUPS, GROUP_WIDTH, GROUP_WIDTH), GROUP_WIDTH ** -0.5, 0.5, ((0, 2),))
    map_balance = jnp.clip(jax.random.uniform(streams_of[6], (HEADS,), jnp.float32, 0.3, 0.8), 0.3, 0.8)
    head_gain = jnp.clip(1.0 + 0.18 * jax.random.normal(streams_of[7], (2 * HEAD_DIM,), jnp.float32), 0.1, 1.9)
    contrast_out_weight = noise(streams_of[8], (2 * HEADS * HEAD_DIM, D), (2 * HEADS * HEAD_DIM + GROUPS * GROUP_WIDTH) ** -0.5, 0.109375, ((0, 2),))
    pool_out_weight = noise(streams_of[9], (GROUPS * GROUP_WIDTH, D), (2 * HEADS * HEAD_DIM + GROUPS * GROUP_WIDTH) ** -0.5, 0.109375, ((0, 2),))
    return {"normed": normed, "query_weight": query_weight, "key_weight": key_weight, "value_weight": value_weight, "pool_in_weight": pool_in_weight, "pool_weight": pool_weight, "map_balance": map_balance, "head_gain": head_gain, "contrast_out_weight": contrast_out_weight, "pool_out_weight": pool_out_weight}


reach_back = 15
norm_epsilon = 1e-06

def map_output(queries, key_rows, value_rows):
    total_rows = queries.shape[0]
    block_rows = math.gcd(total_rows, 1024)
    score_scale = HEAD_DIM ** (-0.5)
    outputs = []
    for block_index in range(total_rows // block_rows):
        first_row = block_index * block_rows
        last_row = first_row + block_rows
        scores = jnp.dot(queries[first_row:last_row], key_rows[:last_row].T, preferred_element_type=jnp.float32) * score_scale
        query_order = first_row + jnp.arange(block_rows, dtype=jnp.int32)
        key_order = jnp.arange(last_row, dtype=jnp.int32)
        scores = jnp.where(key_order[None, :] <= query_order[:, None], scores, -jnp.inf)
        row_peak = lax.optimization_barrier(jnp.max(scores, axis=1, keepdims=True))
        raised = jnp.exp(scores - row_peak)
        row_total = lax.optimization_barrier(jnp.sum(raised, axis=1, keepdims=True))
        weighted = jnp.dot(raised.astype(jnp.bfloat16), value_rows[:last_row], preferred_element_type=jnp.float32)
        outputs.append((weighted / row_total).astype(jnp.bfloat16))
    return jnp.concatenate(outputs, axis=0)

def reference(normed, query_weight, key_weight, value_weight, pool_in_weight, pool_weight, map_balance, head_gain, contrast_out_weight, pool_out_weight):
    queries = jnp.dot(normed, query_weight, preferred_element_type=jnp.float32).astype(jnp.bfloat16)
    key_rows = jnp.dot(normed, key_weight, preferred_element_type=jnp.float32).astype(jnp.bfloat16)
    value_rows = jnp.dot(normed, value_weight, preferred_element_type=jnp.float32).astype(jnp.bfloat16)
    pool_input = jnp.dot(normed, pool_in_weight, preferred_element_type=jnp.float32).astype(jnp.bfloat16)
    value_width = 2 * HEAD_DIM
    head_outputs = []
    for head in range(HEADS):
        maps = []
        for which in range(2):
            column = (2 * head + which) * HEAD_DIM
            result_map = map_output(queries[:, column:column + HEAD_DIM], key_rows[:, column:column + HEAD_DIM], value_rows[:, head * value_width:(head + 1) * value_width])
            maps.append(lax.optimization_barrier(result_map).astype(jnp.float32))
        contrast = maps[0] - map_balance[head] * maps[1]
        mean_square = lax.optimization_barrier(jnp.mean(contrast * contrast, axis=1, keepdims=True))
        head_outputs.append((contrast * lax.rsqrt(mean_square + norm_epsilon) * head_gain).astype(jnp.bfloat16))
    contrast_out = jnp.concatenate(head_outputs, axis=1)
    total_rows = normed.shape[0]
    pool_width = GROUPS * GROUP_WIDTH
    extended = jnp.concatenate([jnp.zeros((reach_back, pool_width), jnp.float32), pool_input.astype(jnp.float32)], axis=0)
    group_index = jnp.arange(pool_width, dtype=jnp.int32) // GROUP_WIDTH
    widths = jnp.left_shift(jnp.int32(2), group_index % 4)
    window_sum = jnp.zeros((total_rows, pool_width), jnp.float32)
    for offset in range(reach_back + 1):
        window_sum = window_sum + extended[reach_back - offset:reach_back - offset + total_rows] * (offset < widths)[None, :].astype(jnp.float32)
    position = jnp.arange(total_rows, dtype=jnp.int32)
    counts = jnp.minimum(position[:, None] + 1, widths[None, :]).astype(jnp.float32)
    spread = (window_sum / counts - extended[reach_back:]).astype(jnp.bfloat16)
    spread = lax.optimization_barrier(spread).astype(jnp.float32)
    mixed_groups = jnp.einsum('sgc,gce->sge', spread.reshape(total_rows, GROUPS, GROUP_WIDTH), pool_weight.astype(jnp.float32))
    pool_out = mixed_groups.reshape(total_rows, pool_width).astype(jnp.bfloat16)
    diff_rows = 2 * HEADS * HEAD_DIM // N_TP
    pool_rows = GROUPS * GROUP_WIDTH // N_TP
    summed = jnp.zeros((total_rows, D), jnp.float32)
    for part_index in range(N_TP):
        low_diff = part_index * diff_rows
        low_pool = part_index * pool_rows
        partial_value = jnp.dot(contrast_out[:, low_diff:low_diff + diff_rows], contrast_out_weight[low_diff:low_diff + diff_rows], preferred_element_type=jnp.float32)
        partial_value = partial_value + jnp.dot(pool_out[:, low_pool:low_pool + pool_rows], pool_out_weight[low_pool:low_pool + pool_rows], preferred_element_type=jnp.float32)
        summed = summed + lax.optimization_barrier(partial_value.astype(jnp.bfloat16)).astype(jnp.float32)
    return summed.astype(jnp.bfloat16)
```

```python
import functools
import math

import jax
import jax.numpy as jnp
from jax import lax
from jax.experimental import pallas as pl
from jax.experimental.pallas import tpu as pltpu
from jax.sharding import PartitionSpec as P

reach_back = 15
norm_epsilon = 1e-06


def passed_along(block, axis, distance):
    devices = range(lax.axis_size(axis))
    route = [(i - distance, i) for i in devices if i - distance in devices]
    return lax.ppermute(block, axis, route)


def from_partner(block, axis, stride):
    count = lax.axis_size(axis)
    route = []
    for low in range(count):
        high = low | 1 << stride
        if high != low and high < count:
            route += [(low, high), (high, low)]
    return lax.ppermute(block, axis, route)


def shifted(array, axis, by):
    size = lax.axis_size(axis)
    return lax.ppermute(array, axis, [(i, (i + by) % size) for i in range(size)])


def as_sent(array):

    def short(part):
        return part.astype(jnp.bfloat16) if part.dtype == jnp.float32 else part

    return jax.tree.map(short, array)


def attend(running, queries, key_rows, value_rows, query_first, key_first, score_scale):
    key_count = key_rows.shape[0]
    key_block = math.gcd(key_count, 1024)
    unit_count = queries.shape[1]
    heads_here = value_rows.shape[1]
    per_head = unit_count // heads_here
    query_count = queries.shape[0]
    query_order = query_first + lax.iota(jnp.int32, query_count)

    def key_step(block_index, carried):
        block_start = block_index * key_block

        def block_work(current):
            row_peak, row_total, weighted = current
            scores = (
                jnp.einsum("qud,kud->uqk", queries, key_rows, preferred_element_type=jnp.float32)
                * score_scale
            )
            key_order = key_first + block_start + lax.iota(jnp.int32, key_block)
            scores = jnp.where(
                key_order[None, None, :] <= query_order[None, :, None], scores, -jnp.inf
            )
            new_peak = jnp.maximum(row_peak, jnp.max(scores, axis=2))
            shrink = jnp.exp(row_peak - new_peak)
            raised = jnp.exp(scores - new_peak[:, :, None])
            row_total = row_total * shrink + jnp.sum(raised, axis=2)
            map_weights = raised.astype(jnp.bfloat16).reshape(
                heads_here, per_head, query_count, key_block
            )
            update = jnp.einsum(
                "hmqk,khe->hmqe", map_weights, value_rows, preferred_element_type=jnp.float32
            )
            weighted = weighted * shrink[:, :, None] + update.reshape(unit_count, query_count, -1)
            return (new_peak, row_total, weighted)

        def keep_state(current):
            return current

        return lax.cond(
            key_first + block_start <= query_first + query_count - 1,
            block_work,
            keep_state,
            carried,
        )

    return lax.fori_loop(0, key_count // key_block, key_step, running)


def fresh_state(unit_count, row_count, value_width):
    return (
        jnp.full((unit_count, row_count), -1e30, jnp.float32),
        jnp.zeros((unit_count, row_count), jnp.float32),
        jnp.zeros((unit_count, row_count, value_width), jnp.float32),
    )


def finished(running):
    row_peak, row_total, weighted = running
    return (weighted / row_total[:, :, None]).astype(jnp.bfloat16)


def joined_state(first, second):
    first_peak, first_total, first_weighted = first
    second_peak, second_total, second_weighted = second
    new_peak = jnp.maximum(first_peak, second_peak)
    first_shrink = jnp.exp(first_peak - new_peak)
    second_shrink = jnp.exp(second_peak - new_peak)
    new_total = first_total * first_shrink + second_total * second_shrink
    new_weighted = (
        first_weighted * first_shrink[:, :, None] + second_weighted * second_shrink[:, :, None]
    )
    return (new_peak, new_total, new_weighted)


def per_device(
    normed,
    query_weight,
    key_weight,
    value_weight,
    pool_in_weight,
    pool_weight,
    map_balance,
    head_gain,
    contrast_out_weight,
    pool_out_weight,
):
    tp_index = lax.axis_index("tp")
    sp_count = lax.axis_size("sp")
    sp_index = lax.axis_index("sp")
    head_dim = head_gain.shape[0] // 2
    value_width = 2 * head_dim
    query_cols = query_weight.shape[1]
    value_cols = value_weight.shape[1]
    unit_count = query_cols // head_dim
    heads_here = unit_count // 2
    project_incoming = lax.all_gather(normed, "tp", axis=0, tiled=True)
    products = [
        jnp.dot(project_incoming, weight_part, preferred_element_type=jnp.float32)
        for weight_part in (query_weight, key_weight, value_weight, pool_in_weight)
    ]
    joined = jnp.concatenate(products, axis=1).astype(jnp.bfloat16)
    row_count = joined.shape[0]
    queries = joined[:, :query_cols].reshape(row_count, unit_count, head_dim)
    key_rows = joined[:, query_cols : 2 * query_cols].reshape(row_count, unit_count, head_dim)
    value_rows = joined[:, 2 * query_cols : 2 * query_cols + value_cols].reshape(
        row_count, heads_here, value_width
    )
    pool_input = joined[:, 2 * query_cols + value_cols :]
    pool_cols = pool_input.shape[1]
    upper_rim = passed_along(pool_input[row_count - reach_back :], "sp", 1)
    extended = jnp.concatenate([upper_rim, pool_input], axis=0).astype(jnp.float32)
    groups_here = pool_weight.shape[0]
    group_width = pool_weight.shape[1]
    group_index = tp_index * groups_here + lax.iota(jnp.int32, pool_cols) // group_width
    widths = jnp.left_shift(jnp.int32(2), group_index % 4)
    window_sum = jnp.zeros((row_count, pool_cols), jnp.float32)
    for offset in range(reach_back + 1):
        window_sum = window_sum + extended[
            reach_back - offset : reach_back - offset + row_count
        ] * (offset < widths)[None, :].astype(jnp.float32)
    position = sp_index * row_count + lax.iota(jnp.int32, row_count)
    counts = jnp.minimum(position[:, None] + 1, widths[None, :]).astype(jnp.float32)
    spread = (window_sum / counts - extended[reach_back:]).astype(jnp.bfloat16)
    mixed_groups = jnp.einsum(
        "tgc,gce->tge",
        spread.reshape(row_count, groups_here, group_width),
        pool_weight,
        preferred_element_type=jnp.float32,
    )
    pool_out = mixed_groups.reshape(row_count, pool_cols).astype(jnp.bfloat16)
    score_scale = head_dim ** (-0.5)
    level_count = sp_count.bit_length() - 1
    low_levels = level_count // 2
    band_size = 1 << low_levels
    band_count = sp_count // band_size
    member = sp_index % band_size
    band = sp_index // band_size
    band_queries = queries
    for bit in range(low_levels):
        received = from_partner(band_queries, "sp", bit)
        upper = member >> bit & 1 == 1
        band_queries = jnp.where(
            upper,
            jnp.concatenate([received, band_queries], axis=0),
            jnp.concatenate([band_queries, received], axis=0),
        )
    band_first = band * band_size * row_count
    running = fresh_state(unit_count, band_size * row_count, value_width)
    for step in range(band_count):
        if step == 0:
            key_piece, value_piece = (key_rows, value_rows)
        else:
            key_piece, value_piece = shifted((key_rows, value_rows), "sp", step * band_size)
        source = (sp_index - step * band_size) % sp_count
        running = attend(
            running,
            band_queries,
            key_piece,
            value_piece,
            band_first,
            source * row_count,
            score_scale,
        )
    for bit in range(low_levels - 1, -1, -1):
        half = running[0].shape[1] // 2
        upper = member >> bit & 1 == 1
        lower_part = jax.tree.map(lambda item: item[:, :half], running)
        upper_part = jax.tree.map(lambda item: item[:, half:], running)
        outgoing = jax.tree.map(
            lambda low, high: jnp.where(upper, low, high), lower_part, upper_part
        )
        kept = jax.tree.map(lambda low, high: jnp.where(upper, high, low), lower_part, upper_part)
        incoming = from_partner(
            (as_sent(outgoing[0]), as_sent(outgoing[1]), as_sent(outgoing[2])), "sp", bit
        )
        running = joined_state(kept, incoming)
    maps = finished(running)
    paired = maps.reshape(heads_here, 2, row_count, value_width)
    paired = lax.optimization_barrier(paired).astype(jnp.float32)
    head_first = tp_index * heads_here
    balance_here = lax.dynamic_slice_in_dim(map_balance, head_first, heads_here, 0)
    contrast = paired[:, 0] - balance_here[:, None, None] * paired[:, 1]
    mean_square = jnp.mean(contrast * contrast, axis=2, keepdims=True)
    contrast = contrast * lax.rsqrt(mean_square + norm_epsilon) * head_gain
    contrast_out = (
        contrast.astype(jnp.bfloat16)
        .transpose(1, 0, 2)
        .reshape(row_count, heads_here * value_width)
    )
    partial_value = jnp.dot(contrast_out, contrast_out_weight, preferred_element_type=jnp.float32)
    return lax.psum_scatter(
        (
            partial_value + jnp.dot(pool_out, pool_out_weight, preferred_element_type=jnp.float32)
        ).astype(jnp.bfloat16),
        "tp",
        scatter_dimension=0,
        tiled=True,
    )


MESH = pl.DeviceIdType.MESH


def flipped(index, mask, size):
    total = 0
    bit = 1
    while bit < size:
        total = total + lax.rem(lax.div(index, bit) + lax.div(mask, bit), 2) * bit
        bit *= 2
    return total


def layer_kernel(
    sp_count,
    members,
    x_ref,
    pool_weight,
    balance,
    gain,
    query_hbm,
    key_hbm,
    value_hbm,
    pool_in_hbm,
    contrast_hbm,
    pool_out_hbm,
    out_ref,
    query_w,
    key_w,
    value_w,
    pool_in_w,
    contrast_w,
    pool_out_w,
    rows_in,
    kv,
    kv_stage,
    queries,
    query_stage,
    peaks,
    totals,
    weighted,
    contrasts,
    contrast_stage,
    rim,
    rim_stage,
    pool_part,
    out_stage,
    out_recv,
    weight_sem,
    local_sem,
    pair_send,
    pair_recv,
    relay_send,
    relay_recv,
    kv_send,
    kv_recv,
    query_send,
    query_recv,
    contrast_send,
    contrast_recv,
    rim_send,
    rim_recv,
    out_send,
    out_recv_sem,
):
    f32 = jnp.float32
    bf16 = jnp.bfloat16
    bands = sp_count // members
    sp = lax.axis_index("sp")
    tp = lax.axis_index("tp")
    other = 1 - tp
    band = lax.div(sp, members)
    member = lax.rem(sp, members)
    half, model = x_ref.shape
    rows = 2 * half
    width = gain.shape[1]
    head_dim = width // 2

    loads = [
        pltpu.make_async_copy(src, dst, weight_sem.at[i])
        for i, (src, dst) in enumerate(
            (
                (key_hbm, key_w),
                (value_hbm, value_w),
                (query_hbm, query_w),
                (pool_in_hbm, pool_in_w),
                (pool_out_hbm, pool_out_w),
                (contrast_hbm, contrast_w),
            )
        )
    ]
    for load in loads:
        load.start()
    keep = pltpu.make_async_copy(x_ref, rows_in.at[0, tp], local_sem)
    keep.start()

    barrier = pltpu.get_barrier_semaphore()
    greeted = [
        (sp, other),
        (lax.rem(sp + members, sp_count), tp),
        (lax.rem(sp + sp_count - members, sp_count), tp),
        (lax.rem(sp + 1, sp_count), tp),
        (lax.rem(sp + sp_count - 1, sp_count), tp),
    ]
    greeted += [(band * members + flipped(member, j, members), tp) for j in range(1, members)]
    for target in greeted:
        pl.semaphore_signal(barrier, inc=1, device_id=target, device_id_type=MESH)
    pl.semaphore_wait(barrier, len(greeted))

    def pair_copy(step):
        return pltpu.make_async_remote_copy(
            src_ref=x_ref if step == 0 else rows_in.at[step, tp],
            dst_ref=rows_in.at[step, tp],
            send_sem=pair_send.at[step],
            recv_sem=pair_recv.at[step],
            device_id=(sp, other),
            device_id_type=MESH,
        )

    def relay_copy(step):
        return pltpu.make_async_remote_copy(
            src_ref=x_ref if step == 1 else rows_in.at[step - 1, tp],
            dst_ref=rows_in.at[step, tp],
            send_sem=relay_send.at[step],
            recv_sem=relay_recv.at[step],
            device_id=(lax.rem(sp + members, sp_count), tp),
            device_id_type=MESH,
        )

    def kv_copy(step, j):
        return pltpu.make_async_remote_copy(
            src_ref=kv_stage.at[step, j],
            dst_ref=kv.at[step, member],
            send_sem=kv_send.at[step, j],
            recv_sem=kv_recv.at[step, j],
            device_id=(band * members + flipped(member, j, members), tp),
            device_id_type=MESH,
        )

    def query_copy(j):
        return pltpu.make_async_remote_copy(
            src_ref=query_stage.at[j],
            dst_ref=queries.at[member],
            send_sem=query_send.at[j],
            recv_sem=query_recv.at[j],
            device_id=(band * members + flipped(member, j, members), tp),
            device_id_type=MESH,
        )

    def contrast_copy(j):
        return pltpu.make_async_remote_copy(
            src_ref=contrast_stage.at[j],
            dst_ref=contrasts.at[member],
            send_sem=contrast_send.at[j],
            recv_sem=contrast_recv.at[j],
            device_id=(band * members + flipped(member, j, members), tp),
            device_id_type=MESH,
        )

    rim_copy = pltpu.make_async_remote_copy(
        src_ref=rim_stage,
        dst_ref=rim,
        send_sem=rim_send,
        recv_sem=rim_recv,
        device_id=(lax.rem(sp + 1, sp_count), tp),
        device_id_type=MESH,
    )
    out_copy = pltpu.make_async_remote_copy(
        src_ref=out_stage,
        dst_ref=out_recv,
        send_sem=out_send,
        recv_sem=out_recv_sem,
        device_id=(sp, other),
        device_id_type=MESH,
    )

    pair_copy(0).start()

    @pl.when(band + 1 < bands)
    def _():
        relay_copy(1).start()

    def project(step):
        def one(t, carry):
            j = members - 1 - t
            head = flipped(member, j, members)
            columns = pl.ds(pl.multiple_of(head * width, width), width)
            x = rows_in[step].reshape(rows, model)
            keys = jnp.dot(x, key_w[:, columns], preferred_element_type=f32).astype(bf16)
            values = jnp.dot(x, value_w[:, columns], preferred_element_type=f32).astype(bf16)

            @pl.when(j > 0)
            def _():
                kv_stage[step, j, :, :width] = keys
                kv_stage[step, j, :, width:] = values
                kv_copy(step, j).start()

            @pl.when(j == 0)
            def _():
                kv[step, member, :, :width] = keys
                kv[step, member, :, width:] = values

            if step == 0:
                mine = jnp.dot(x, query_w[:, columns], preferred_element_type=f32).astype(bf16)

                @pl.when(j > 0)
                def _():
                    query_stage[j] = mine
                    query_copy(j).start()

                @pl.when(j == 0)
                def _():
                    queries[member] = mine

            return carry

        lax.fori_loop(0, members, one, 0)

    def take_band(step):
        @pl.when(band >= step)
        def _():
            relay_copy(step).wait_recv()
            if step + 1 < bands:

                @pl.when(band + 1 < bands)
                def _():
                    relay_copy(step + 1).start()

            pair_copy(step).start()
            pair_copy(step).wait_recv()
            project(step)

    log_scale = head_dim ** (-0.5) * math.log2(math.e)

    def attend_block(step, i, seen):
        for u in range(2):
            cols = slice(u * head_dim, (u + 1) * head_dim)
            keys = kv[step, :seen, :, cols].reshape(seen * rows, head_dim)
            values = kv[step, :seen, :, width:].reshape(seen * rows, width)
            scores = lax.dot_general(
                queries[i, :, cols], keys, (((1,), (1,)), ((), ())), preferred_element_type=f32
            )
            if step == 0:
                query_order = lax.broadcasted_iota(jnp.int32, scores.shape, 0) + (seen - 1) * rows
                key_order = lax.broadcasted_iota(jnp.int32, scores.shape, 1)
                scores = jnp.where(key_order <= query_order, scores, -jnp.inf)
            peak = jnp.max(scores, axis=1, keepdims=True)
            if step > 0:
                old = peaks[u, i][:, :1]
                peak = jnp.maximum(peak, old)
                shrink = jnp.exp2((old - peak) * log_scale)
            raised = jnp.exp2((scores - peak) * log_scale)
            total = jnp.sum(raised, axis=1, keepdims=True)
            update = jnp.dot(raised.astype(bf16), values, preferred_element_type=f32)
            if step > 0:
                total = total + totals[u, i][:, :1] * shrink
                update = update + weighted[u, i] * shrink
            peaks[u, i] = jnp.broadcast_to(peak, peaks.shape[2:])
            totals[u, i] = jnp.broadcast_to(total, totals.shape[2:])
            weighted[u, i] = update

    def attend_own():
        for j in range(1, members):
            query_copy(j).wait_recv()
            kv_copy(0, j).wait_recv()
        for i in range(members):
            attend_block(0, i, i + 1)

    def attend_band(step):
        @pl.when(band >= step)
        def _():
            for j in range(1, members):
                kv_copy(step, j).wait_recv()

            def one(i, carry):
                attend_block(step, i, members)
                return carry

            lax.fori_loop(0, members, one, 0)

    keep.wait()
    loads[0].wait()
    loads[1].wait()
    loads[2].wait()
    pair_copy(0).wait_recv()
    project(0)

    loads[3].wait()
    pool_input = jnp.dot(
        rows_in[0].reshape(rows, model), pool_in_w[...], preferred_element_type=f32
    ).astype(bf16)
    rim_stage[...] = pool_input[rows - rim.shape[0] :]

    @pl.when(sp + 1 < sp_count)
    def _():
        rim_copy.start()

    take_band(1)

    @pl.when(sp > 0)
    def _():
        rim_copy.wait_recv()

    @pl.when(sp == 0)
    def _():
        rim[...] = jnp.zeros_like(rim)

    loads[4].wait()
    extended = jnp.concatenate([rim[...], pool_input], axis=0).astype(f32)
    group_width = pool_weight.shape[1]
    skirt = rim.shape[0]
    position = sp * rows + lax.broadcasted_iota(jnp.int32, (rows, group_width), 0)
    mixed = []
    for group in range(pool_weight.shape[0]):
        block = extended[:, group * group_width : (group + 1) * group_width]
        window = block
        reach = 1
        span = 2 ** (1 + group % 4)
        while reach < span:
            window = window + pltpu.roll(window, reach, 0)
            reach *= 2
        counts = jnp.minimum(position + 1, span).astype(f32)
        spread = (window[skirt:] / counts - block[skirt:]).astype(bf16)
        mixed.append(
            jnp.dot(spread, pool_weight[group], preferred_element_type=f32).astype(bf16)
        )
    pool_out = jnp.concatenate(mixed, axis=1)
    chunk = math.gcd(model, 512)
    for start in range(0, model, chunk):
        pool_part[:, start : start + chunk] = jnp.dot(
            pool_out, pool_out_w[:, start : start + chunk], preferred_element_type=f32
        )

    for step in range(2, bands):
        take_band(step)
        if step == 2:
            attend_own()
        else:
            attend_band(step - 2)
    if bands == 2:
        attend_own()
    for step in range(max(bands - 2, 1), bands):
        attend_band(step)

    weight = balance[tp * members + member]

    def finish(t, carry):
        j = members - 1 - t
        i = flipped(member, j, members)
        first = (weighted[0, i] / totals[0, i][:, :1]).astype(bf16).astype(f32)
        second = (weighted[1, i] / totals[1, i][:, :1]).astype(bf16).astype(f32)
        contrast = first - weight * second
        mean_square = jnp.mean(contrast * contrast, axis=1, keepdims=True)
        result = (contrast * lax.rsqrt(mean_square + norm_epsilon) * gain[...]).astype(bf16)

        @pl.when(j > 0)
        def _():
            contrast_stage[j] = result
            contrast_copy(j).start()

        @pl.when(j == 0)
        def _():
            contrasts[member] = result

        return carry

    lax.fori_loop(0, members, finish, 0)
    loads[5].wait()
    for j in range(1, members):
        contrast_copy(j).wait_recv()

    def projected(side, store):
        taken = pl.ds(pl.multiple_of(side * half, half), half)
        left = jnp.concatenate([contrasts[h, taken, :] for h in range(members)], axis=1)
        for start in range(0, model, chunk):
            cut = slice(start, start + chunk)
            part = jnp.dot(left, contrast_w[:, cut], preferred_element_type=f32)
            store(cut, (part + pool_part[taken, cut]).astype(bf16))

    def to_partner(cut, part):
        out_stage[:, cut] = part

    def to_self(cut, part):
        out_ref[:, cut] = part

    projected(other, to_partner)
    out_copy.start()
    projected(tp, to_self)
    out_copy.wait()
    out_ref[...] = (out_ref[...].astype(f32) + out_recv[...].astype(f32)).astype(bf16)

    pair_copy(0).wait_send()
    for j in range(1, members):
        query_copy(j).wait_send()
        kv_copy(0, j).wait_send()
        contrast_copy(j).wait_send()

    @pl.when(sp + 1 < sp_count)
    def _():
        rim_copy.wait_send()

    for step in range(1, bands):

        @pl.when(jnp.logical_and(band + 1 < bands, band >= step - 1))
        def _(step=step):
            relay_copy(step).wait_send()

        @pl.when(band >= step)
        def _(step=step):
            pair_copy(step).wait_send()
            for j in range(1, members):
                kv_copy(step, j).wait_send()


def kernel_scratch(sp_count, members, half, model, width, pool_cols):
    bf16 = jnp.bfloat16
    bands = sp_count // members
    rows = 2 * half
    columns = members * width
    dma = pltpu.SemaphoreType.DMA
    return [
        pltpu.VMEM((model, columns), bf16),
        pltpu.VMEM((model, columns), bf16),
        pltpu.VMEM((model, columns), bf16),
        pltpu.VMEM((model, pool_cols), bf16),
        pltpu.VMEM((columns, model), bf16),
        pltpu.VMEM((pool_cols, model), bf16),
        pltpu.VMEM((bands, 2, half, model), bf16),
        pltpu.VMEM((bands, members, rows, 2 * width), bf16),
        pltpu.VMEM((bands, members, rows, 2 * width), bf16),
        pltpu.VMEM((members, rows, width), bf16),
        pltpu.VMEM((members, rows, width), bf16),
        pltpu.VMEM((2, members, rows, 128), jnp.float32),
        pltpu.VMEM((2, members, rows, 128), jnp.float32),
        pltpu.VMEM((2, members, rows, width), jnp.float32),
        pltpu.VMEM((members, rows, width), bf16),
        pltpu.VMEM((members, rows, width), bf16),
        pltpu.VMEM((reach_back + 1, pool_cols), bf16),
        pltpu.VMEM((reach_back + 1, pool_cols), bf16),
        pltpu.VMEM((rows, model), jnp.float32),
        pltpu.VMEM((half, model), bf16),
        pltpu.VMEM((half, model), bf16),
        dma((6,)),
        dma,
        dma((bands,)),
        dma((bands,)),
        dma((bands,)),
        dma((bands,)),
        dma((bands, members)),
        dma((bands, members)),
        dma((members,)),
        dma((members,)),
        dma((members,)),
        dma((members,)),
        dma,
        dma,
        dma,
        dma,
    ]


vmem_most = 67043328


def scratch_bytes(scratch):
    return sum(
        math.prod(item.shape) * jnp.dtype(item.dtype).itemsize
        for item in scratch
        if getattr(item, "memory_space", None) == pltpu.VMEM
    )


def whole_layer(
    normed,
    query_weight,
    key_weight,
    value_weight,
    pool_in_weight,
    pool_weight,
    map_balance,
    head_gain,
    contrast_out_weight,
    pool_out_weight,
):
    sp_count = lax.axis_size("sp")
    width = head_gain.shape[0]
    members = query_weight.shape[1] // width
    half, model = normed.shape
    pool_cols = pool_in_weight.shape[1]
    groups_here = pool_weight.shape[0]
    scratch = kernel_scratch(
        sp_count, max(members, 1), half, model, width, pool_cols
    )
    fits = (
        lax.axis_size("tp") == 2
        and members > 1
        and members & (members - 1) == 0
        and sp_count % members == 0
        and sp_count // members > 1
        and groups_here % 4 == 0
        and scratch_bytes(scratch) < vmem_most * 3 // 4
    )
    if not fits:
        return per_device(
            normed,
            query_weight,
            key_weight,
            value_weight,
            pool_in_weight,
            pool_weight,
            map_balance,
            head_gain,
            contrast_out_weight,
            pool_out_weight,
        )
    vmem = pl.BlockSpec(memory_space=pltpu.VMEM)
    hbm = pl.BlockSpec(memory_space=pl.ANY)
    return pl.pallas_call(
        functools.partial(layer_kernel, sp_count, members),
        out_shape=jax.ShapeDtypeStruct((half, model), jnp.bfloat16),
        in_specs=[vmem, vmem, pl.BlockSpec(memory_space=pltpu.SMEM), vmem] + [hbm] * 6,
        out_specs=vmem,
        scratch_shapes=scratch,
        compiler_params=pltpu.CompilerParams(
            collective_id=0, has_side_effects=True, vmem_limit_bytes=vmem_most
        ),
    )(
        normed,
        pool_weight,
        map_balance,
        head_gain.reshape(1, width),
        query_weight,
        key_weight,
        value_weight,
        pool_in_weight,
        contrast_out_weight,
        pool_out_weight,
    )


def solution(mesh):
    return jax.shard_map(
        whole_layer,
        mesh=mesh,
        in_specs=(
            P(("sp", "tp"), None),
            P(None, "tp"),
            P(None, "tp"),
            P(None, "tp"),
            P(None, "tp"),
            P("tp", None, None),
            P(),
            P(),
            P("tp", None),
            P("tp", None),
        ),
        out_specs=P(("sp", "tp"), None),
        check_vma=False,
    )
```

```python
import functools
import math

import jax
import jax.numpy as jnp
from jax import lax
from jax.experimental import pallas as pl
from jax.experimental.pallas import tpu as pltpu
from jax.sharding import PartitionSpec as P

reach_back = 15
norm_epsilon = 1e-06


def passed_along(block, axis, distance):
    devices = range(lax.axis_size(axis))
    route = [(i - distance, i) for i in devices if i - distance in devices]
    return lax.ppermute(block, axis, route)


def from_partner(block, axis, stride):
    count = lax.axis_size(axis)
    route = []
    for low in range(count):
        high = low | 1 << stride
        if high != low and high < count:
            route += [(low, high), (high, low)]
    return lax.ppermute(block, axis, route)


def shifted(array, axis, by):
    size = lax.axis_size(axis)
    return lax.ppermute(array, axis, [(i, (i + by) % size) for i in range(size)])


def as_sent(array):

    def short(part):
        return part.astype(jnp.bfloat16) if part.dtype == jnp.float32 else part

    return jax.tree.map(short, array)


def attend(running, queries, key_rows, value_rows, query_first, key_first, score_scale):
    key_count = key_rows.shape[0]
    key_block = math.gcd(key_count, 1024)
    unit_count = queries.shape[1]
    heads_here = value_rows.shape[1]
    per_head = unit_count // heads_here
    query_count = queries.shape[0]
    query_order = query_first + lax.iota(jnp.int32, query_count)

    def key_step(block_index, carried):
        block_start = block_index * key_block

        def block_work(current):
            row_peak, row_total, weighted = current
            scores = (
                jnp.einsum("qud,kud->uqk", queries, key_rows, preferred_element_type=jnp.float32)
                * score_scale
            )
            key_order = key_first + block_start + lax.iota(jnp.int32, key_block)
            scores = jnp.where(
                key_order[None, None, :] <= query_order[None, :, None], scores, -jnp.inf
            )
            new_peak = jnp.maximum(row_peak, jnp.max(scores, axis=2))
            shrink = jnp.exp(row_peak - new_peak)
            raised = jnp.exp(scores - new_peak[:, :, None])
            row_total = row_total * shrink + jnp.sum(raised, axis=2)
            map_weights = raised.astype(jnp.bfloat16).reshape(
                heads_here, per_head, query_count, key_block
            )
            update = jnp.einsum(
                "hmqk,khe->hmqe", map_weights, value_rows, preferred_element_type=jnp.float32
            )
            weighted = weighted * shrink[:, :, None] + update.reshape(unit_count, query_count, -1)
            return (new_peak, row_total, weighted)

        def keep_state(current):
            return current

        return lax.cond(
            key_first + block_start <= query_first + query_count - 1,
            block_work,
            keep_state,
            carried,
        )

    return lax.fori_loop(0, key_count // key_block, key_step, running)


def fresh_state(unit_count, row_count, value_width):
    return (
        jnp.full((unit_count, row_count), -1e30, jnp.float32),
        jnp.zeros((unit_count, row_count), jnp.float32),
        jnp.zeros((unit_count, row_count, value_width), jnp.float32),
    )


def finished(running):
    row_peak, row_total, weighted = running
    return (weighted / row_total[:, :, None]).astype(jnp.bfloat16)


def joined_state(first, second):
    first_peak, first_total, first_weighted = first
    second_peak, second_total, second_weighted = second
    new_peak = jnp.maximum(first_peak, second_peak)
    first_shrink = jnp.exp(first_peak - new_peak)
    second_shrink = jnp.exp(second_peak - new_peak)
    new_total = first_total * first_shrink + second_total * second_shrink
    new_weighted = (
        first_weighted * first_shrink[:, :, None] + second_weighted * second_shrink[:, :, None]
    )
    return (new_peak, new_total, new_weighted)


def per_device(
    normed,
    query_weight,
    key_weight,
    value_weight,
    pool_in_weight,
    pool_weight,
    map_balance,
    head_gain,
    contrast_out_weight,
    pool_out_weight,
):
    tp_index = lax.axis_index("tp")
    sp_count = lax.axis_size("sp")
    sp_index = lax.axis_index("sp")
    head_dim = head_gain.shape[0] // 2
    value_width = 2 * head_dim
    query_cols = query_weight.shape[1]
    value_cols = value_weight.shape[1]
    unit_count = query_cols // head_dim
    heads_here = unit_count // 2
    project_incoming = lax.all_gather(normed, "tp", axis=0, tiled=True)
    products = [
        jnp.dot(project_incoming, weight_part, preferred_element_type=jnp.float32)
        for weight_part in (query_weight, key_weight, value_weight, pool_in_weight)
    ]
    joined = jnp.concatenate(products, axis=1).astype(jnp.bfloat16)
    row_count = joined.shape[0]
    queries = joined[:, :query_cols].reshape(row_count, unit_count, head_dim)
    key_rows = joined[:, query_cols : 2 * query_cols].reshape(row_count, unit_count, head_dim)
    value_rows = joined[:, 2 * query_cols : 2 * query_cols + value_cols].reshape(
        row_count, heads_here, value_width
    )
    pool_input = joined[:, 2 * query_cols + value_cols :]
    pool_cols = pool_input.shape[1]
    upper_rim = passed_along(pool_input[row_count - reach_back :], "sp", 1)
    extended = jnp.concatenate([upper_rim, pool_input], axis=0).astype(jnp.float32)
    groups_here = pool_weight.shape[0]
    group_width = pool_weight.shape[1]
    group_index = tp_index * groups_here + lax.iota(jnp.int32, pool_cols) // group_width
    widths = jnp.left_shift(jnp.int32(2), group_index % 4)
    window_sum = jnp.zeros((row_count, pool_cols), jnp.float32)
    for offset in range(reach_back + 1):
        window_sum = window_sum + extended[
            reach_back - offset : reach_back - offset + row_count
        ] * (offset < widths)[None, :].astype(jnp.float32)
    position = sp_index * row_count + lax.iota(jnp.int32, row_count)
    counts = jnp.minimum(position[:, None] + 1, widths[None, :]).astype(jnp.float32)
    spread = (window_sum / counts - extended[reach_back:]).astype(jnp.bfloat16)
    mixed_groups = jnp.einsum(
        "tgc,gce->tge",
        spread.reshape(row_count, groups_here, group_width),
        pool_weight,
        preferred_element_type=jnp.float32,
    )
    pool_out = mixed_groups.reshape(row_count, pool_cols).astype(jnp.bfloat16)
    score_scale = head_dim ** (-0.5)
    level_count = sp_count.bit_length() - 1
    low_levels = level_count // 2
    band_size = 1 << low_levels
    band_count = sp_count // band_size
    member = sp_index % band_size
    band = sp_index // band_size
    band_queries = queries
    for bit in range(low_levels):
        received = from_partner(band_queries, "sp", bit)
        upper = member >> bit & 1 == 1
        band_queries = jnp.where(
            upper,
            jnp.concatenate([received, band_queries], axis=0),
            jnp.concatenate([band_queries, received], axis=0),
        )
    band_first = band * band_size * row_count
    running = fresh_state(unit_count, band_size * row_count, value_width)
    for step in range(band_count):
        if step == 0:
            key_piece, value_piece = (key_rows, value_rows)
        else:
            key_piece, value_piece = shifted((key_rows, value_rows), "sp", step * band_size)
        source = (sp_index - step * band_size) % sp_count
        running = attend(
            running,
            band_queries,
            key_piece,
            value_piece,
            band_first,
            source * row_count,
            score_scale,
        )
    for bit in range(low_levels - 1, -1, -1):
        half = running[0].shape[1] // 2
        upper = member >> bit & 1 == 1
        lower_part = jax.tree.map(lambda item: item[:, :half], running)
        upper_part = jax.tree.map(lambda item: item[:, half:], running)
        outgoing = jax.tree.map(
            lambda low, high: jnp.where(upper, low, high), lower_part, upper_part
        )
        kept = jax.tree.map(lambda low, high: jnp.where(upper, high, low), lower_part, upper_part)
        incoming = from_partner(
            (as_sent(outgoing[0]), as_sent(outgoing[1]), as_sent(outgoing[2])), "sp", bit
        )
        running = joined_state(kept, incoming)
    maps = finished(running)
    paired = maps.reshape(heads_here, 2, row_count, value_width)
    paired = lax.optimization_barrier(paired).astype(jnp.float32)
    head_first = tp_index * heads_here
    balance_here = lax.dynamic_slice_in_dim(map_balance, head_first, heads_here, 0)
    contrast = paired[:, 0] - balance_here[:, None, None] * paired[:, 1]
    mean_square = jnp.mean(contrast * contrast, axis=2, keepdims=True)
    contrast = contrast * lax.rsqrt(mean_square + norm_epsilon) * head_gain
    contrast_out = (
        contrast.astype(jnp.bfloat16)
        .transpose(1, 0, 2)
        .reshape(row_count, heads_here * value_width)
    )
    partial_value = jnp.dot(contrast_out, contrast_out_weight, preferred_element_type=jnp.float32)
    return lax.psum_scatter(
        (
            partial_value + jnp.dot(pool_out, pool_out_weight, preferred_element_type=jnp.float32)
        ).astype(jnp.bfloat16),
        "tp",
        scatter_dimension=0,
        tiled=True,
    )


MESH = pl.DeviceIdType.MESH


def flipped(index, mask, size):
    total = 0
    bit = 1
    while bit < size:
        total = total + lax.rem(lax.div(index, bit) + lax.div(mask, bit), 2) * bit
        bit *= 2
    return total


def layer_kernel(
    sp_count,
    members,
    x_ref,
    pool_weight,
    balance,
    gain,
    query_hbm,
    key_hbm,
    value_hbm,
    pool_in_hbm,
    contrast_hbm,
    pool_out_hbm,
    out_ref,
    out_recv,
    query_w,
    key_w,
    value_w,
    pool_in_w,
    contrast_w,
    pool_out_w,
    rows_in,
    kv,
    kv_stage,
    queries,
    query_stage,
    peaks,
    totals,
    weighted,
    contrasts,
    contrast_stage,
    rim,
    rim_stage,
    pool_part,
    out_stage,
    weight_sem,
    local_sem,
    pair_send,
    pair_recv,
    relay_send,
    relay_recv,
    kv_send,
    kv_recv,
    query_send,
    query_recv,
    contrast_send,
    contrast_recv,
    rim_send,
    rim_recv,
    out_send,
    out_recv_sem,
):
    f32 = jnp.float32
    bf16 = jnp.bfloat16
    bands = sp_count // members
    sp = lax.axis_index("sp")
    tp = lax.axis_index("tp")
    other = 1 - tp
    band = lax.div(sp, members)
    member = lax.rem(sp, members)
    half, model = x_ref.shape
    rows = 2 * half
    width = gain.shape[1]
    head_dim = width // 2

    loads = [
        pltpu.make_async_copy(src, dst, weight_sem.at[i])
        for i, (src, dst) in enumerate(
            (
                (key_hbm, key_w),
                (value_hbm, value_w),
                (query_hbm, query_w),
                (pool_in_hbm, pool_in_w),
                (pool_out_hbm, pool_out_w),
                (contrast_hbm, contrast_w),
            )
        )
    ]
    for load in loads:
        load.start()
    keep = pltpu.make_async_copy(x_ref, rows_in.at[0, tp], local_sem)
    keep.start()

    barrier = pltpu.get_barrier_semaphore()
    greeted = [
        (sp, other),
        (lax.rem(sp + members, sp_count), tp),
        (lax.rem(sp + sp_count - members, sp_count), tp),
        (lax.rem(sp + 1, sp_count), tp),
        (lax.rem(sp + sp_count - 1, sp_count), tp),
    ]
    greeted += [(band * members + flipped(member, j, members), tp) for j in range(1, members)]
    for target in greeted:
        pl.semaphore_signal(barrier, inc=1, device_id=target, device_id_type=MESH)
    pl.semaphore_wait(barrier, len(greeted))

    def pair_copy(step):
        return pltpu.make_async_remote_copy(
            src_ref=x_ref if step == 0 else rows_in.at[step, tp],
            dst_ref=rows_in.at[step, tp],
            send_sem=pair_send.at[step],
            recv_sem=pair_recv.at[step],
            device_id=(sp, other),
            device_id_type=MESH,
        )

    def relay_copy(step):
        return pltpu.make_async_remote_copy(
            src_ref=x_ref if step == 1 else rows_in.at[step - 1, tp],
            dst_ref=rows_in.at[step, tp],
            send_sem=relay_send.at[step],
            recv_sem=relay_recv.at[step],
            device_id=(lax.rem(sp + members, sp_count), tp),
            device_id_type=MESH,
        )

    def kv_copy(step, j):
        return pltpu.make_async_remote_copy(
            src_ref=kv_stage.at[step, j],
            dst_ref=kv.at[step, member],
            send_sem=kv_send.at[step, j],
            recv_sem=kv_recv.at[step, j],
            device_id=(band * members + flipped(member, j, members), tp),
            device_id_type=MESH,
        )

    def query_copy(j):
        return pltpu.make_async_remote_copy(
            src_ref=query_stage.at[j],
            dst_ref=queries.at[member],
            send_sem=query_send.at[j],
            recv_sem=query_recv.at[j],
            device_id=(band * members + flipped(member, j, members), tp),
            device_id_type=MESH,
        )

    def contrast_copy(j):
        return pltpu.make_async_remote_copy(
            src_ref=contrast_stage.at[j],
            dst_ref=contrasts.at[member],
            send_sem=contrast_send.at[j],
            recv_sem=contrast_recv.at[j],
            device_id=(band * members + flipped(member, j, members), tp),
            device_id_type=MESH,
        )

    rim_copy = pltpu.make_async_remote_copy(
        src_ref=rim_stage,
        dst_ref=rim,
        send_sem=rim_send,
        recv_sem=rim_recv,
        device_id=(lax.rem(sp + 1, sp_count), tp),
        device_id_type=MESH,
    )
    out_copy = pltpu.make_async_remote_copy(
        src_ref=out_stage,
        dst_ref=out_recv,
        send_sem=out_send,
        recv_sem=out_recv_sem,
        device_id=(sp, other),
        device_id_type=MESH,
    )

    pair_copy(0).start()

    @pl.when(band + 1 < bands)
    def _():
        relay_copy(1).start()

    def project(step):
        def one(t, carry):
            j = members - 1 - t
            head = flipped(member, j, members)
            columns = pl.ds(pl.multiple_of(head * width, width), width)
            x = rows_in[step].reshape(rows, model)
            keys = jnp.dot(x, key_w[:, columns], preferred_element_type=f32).astype(bf16)
            values = jnp.dot(x, value_w[:, columns], preferred_element_type=f32).astype(bf16)

            @pl.when(j > 0)
            def _():
                kv_stage[step, j, :, :width] = keys
                kv_stage[step, j, :, width:] = values
                kv_copy(step, j).start()

            @pl.when(j == 0)
            def _():
                kv[step, member, :, :width] = keys
                kv[step, member, :, width:] = values

            if step == 0:
                mine = jnp.dot(x, query_w[:, columns], preferred_element_type=f32).astype(bf16)

                @pl.when(j > 0)
                def _():
                    query_stage[j] = mine
                    query_copy(j).start()

                @pl.when(j == 0)
                def _():
                    queries[member] = mine

            return carry

        lax.fori_loop(0, members, one, 0)

    def take_band(step):
        @pl.when(band >= step)
        def _():
            relay_copy(step).wait_recv()
            if step + 1 < bands:

                @pl.when(band + 1 < bands)
                def _():
                    relay_copy(step + 1).start()

            pair_copy(step).start()
            pair_copy(step).wait_recv()
            project(step)

    log_scale = head_dim ** (-0.5) * math.log2(math.e)

    def attend_block(step, i, blocks):
        seen = len(blocks)
        for u in range(2):
            cols = slice(u * head_dim, (u + 1) * head_dim)
            keys = jnp.concatenate([kv[step, b, :, cols] for b in blocks], axis=0)
            values = jnp.concatenate([kv[step, b, :, width:] for b in blocks], axis=0)
            scores = lax.dot_general(
                queries[i, :, cols], keys, (((1,), (1,)), ((), ())), preferred_element_type=f32
            )
            if step == 0:
                query_order = lax.broadcasted_iota(jnp.int32, scores.shape, 0) + (seen - 1) * rows
                key_order = lax.broadcasted_iota(jnp.int32, scores.shape, 1)
                scores = jnp.where(key_order <= query_order, scores, -jnp.inf)
            peak = jnp.max(scores, axis=1, keepdims=True)
            if step > 0:
                old = peaks[u, i][:, :1]
                peak = jnp.maximum(peak, old)
                shrink = jnp.exp2((old - peak) * log_scale)
            raised = jnp.exp2((scores - peak) * log_scale)
            total = jnp.sum(raised, axis=1, keepdims=True)
            update = jnp.dot(raised.astype(bf16), values, preferred_element_type=f32)
            if step > 0:
                total = total + totals[u, i][:, :1] * shrink
                update = update + weighted[u, i] * shrink
            peaks[u, i] = jnp.broadcast_to(peak, peaks.shape[2:])
            totals[u, i] = jnp.broadcast_to(total, totals.shape[2:])
            weighted[u, i] = update

    weight = balance[tp * members + member]

    def finish(i, j):
        first = (weighted[0, i] / totals[0, i][:, :1]).astype(bf16).astype(f32)
        second = (weighted[1, i] / totals[1, i][:, :1]).astype(bf16).astype(f32)
        contrast = first - weight * second
        mean_square = jnp.mean(contrast * contrast, axis=1, keepdims=True)
        result = (contrast * lax.rsqrt(mean_square + norm_epsilon) * gain[...]).astype(bf16)

        @pl.when(j > 0)
        def _():
            contrast_stage[j] = result
            contrast_copy(j).start()

        @pl.when(j == 0)
        def _():
            contrasts[member] = result

    def attend_own():
        for j in range(1, members):
            query_copy(j).wait_recv()
            kv_copy(0, j).wait_recv()
        for i in range(members):
            attend_block(0, i, list(range(i + 1)))

            @pl.when(band == 0)
            def _(i=i):
                finish(i, flipped(member, i, members))

    early = [0] + list(range(members // 2 + 1, members))
    late = [j for j in range(1, members) if j not in early]

    def attend_band(step):
        @pl.when(band >= step)
        def _():
            for part in (early, late):
                for j in part:
                    if j > 0:
                        kv_copy(step, j).wait_recv()
                blocks = [flipped(member, j, members) for j in part]

                def one(t, carry, part=part, blocks=blocks):
                    j = members - 1 - t
                    i = flipped(member, j, members)
                    attend_block(step, i, blocks)
                    if part is late:

                        @pl.when(band == step)
                        def _():
                            finish(i, j)

                    return carry

                lax.fori_loop(0, members, one, 0)

    keep.wait()
    loads[0].wait()
    loads[1].wait()
    loads[2].wait()
    pair_copy(0).wait_recv()
    project(0)

    loads[3].wait()
    pool_input = jnp.dot(
        rows_in[0].reshape(rows, model), pool_in_w[...], preferred_element_type=f32
    ).astype(bf16)
    rim_stage[...] = pool_input[rows - rim.shape[0] :]

    @pl.when(sp + 1 < sp_count)
    def _():
        rim_copy.start()

    take_band(1)

    @pl.when(sp > 0)
    def _():
        rim_copy.wait_recv()

    @pl.when(sp == 0)
    def _():
        rim[...] = jnp.zeros_like(rim)

    loads[4].wait()
    extended = jnp.concatenate([rim[...], pool_input], axis=0).astype(f32)
    group_width = pool_weight.shape[1]
    skirt = rim.shape[0]
    position = sp * rows + lax.broadcasted_iota(jnp.int32, (rows, group_width), 0)
    mixed = []
    for group in range(pool_weight.shape[0]):
        block = extended[:, group * group_width : (group + 1) * group_width]
        window = block
        reach = 1
        span = 2 ** (1 + group % 4)
        while reach < span:
            window = window + pltpu.roll(window, reach, 0)
            reach *= 2
        counts = jnp.minimum(position + 1, span).astype(f32)
        spread = (window[skirt:] / counts - block[skirt:]).astype(bf16)
        mixed.append(
            jnp.dot(spread, pool_weight[group], preferred_element_type=f32).astype(bf16)
        )
    pool_out = jnp.concatenate(mixed, axis=1)
    chunk = math.gcd(model, 512)
    for start in range(0, model, chunk):
        pool_part[:, start : start + chunk] = jnp.dot(
            pool_out, pool_out_w[:, start : start + chunk], preferred_element_type=f32
        )

    for step in range(2, bands):
        take_band(step)
        if step == 2:
            attend_own()
        else:
            attend_band(step - 2)
    if bands == 2:
        attend_own()
    for step in range(max(bands - 2, 1), bands):
        attend_band(step)

    loads[5].wait()
    for j in range(1, members):
        contrast_copy(j).wait_recv()

    def projected(side, store):
        taken = pl.ds(pl.multiple_of(side * half, half), half)
        left = jnp.concatenate([contrasts[h, taken, :] for h in range(members)], axis=1)
        for start in range(0, model, chunk):
            cut = slice(start, start + chunk)
            part = jnp.dot(left, contrast_w[:, cut], preferred_element_type=f32)
            store(cut, (part + pool_part[taken, cut]).astype(bf16))

    def to_partner(cut, part):
        out_stage[:, cut] = part

    def to_self(cut, part):
        out_ref[:, cut] = part

    projected(other, to_partner)
    out_copy.start()
    projected(tp, to_self)
    out_copy.wait()
    pair_copy(0).wait_send()
    for j in range(1, members):
        query_copy(j).wait_send()
        kv_copy(0, j).wait_send()
        contrast_copy(j).wait_send()

    @pl.when(sp + 1 < sp_count)
    def _():
        rim_copy.wait_send()

    for step in range(1, bands):

        @pl.when(jnp.logical_and(band + 1 < bands, band >= step - 1))
        def _(step=step):
            relay_copy(step).wait_send()

        @pl.when(band >= step)
        def _(step=step):
            pair_copy(step).wait_send()
            for j in range(1, members):
                kv_copy(step, j).wait_send()


def kernel_scratch(sp_count, members, half, model, width, pool_cols):
    bf16 = jnp.bfloat16
    bands = sp_count // members
    rows = 2 * half
    columns = members * width
    dma = pltpu.SemaphoreType.DMA
    return [
        pltpu.VMEM((model, columns), bf16),
        pltpu.VMEM((model, columns), bf16),
        pltpu.VMEM((model, columns), bf16),
        pltpu.VMEM((model, pool_cols), bf16),
        pltpu.VMEM((columns, model), bf16),
        pltpu.VMEM((pool_cols, model), bf16),
        pltpu.VMEM((bands, 2, half, model), bf16),
        pltpu.VMEM((bands, members, rows, 2 * width), bf16),
        pltpu.VMEM((bands, members, rows, 2 * width), bf16),
        pltpu.VMEM((members, rows, width), bf16),
        pltpu.VMEM((members, rows, width), bf16),
        pltpu.VMEM((2, members, rows, 128), jnp.float32),
        pltpu.VMEM((2, members, rows, 128), jnp.float32),
        pltpu.VMEM((2, members, rows, width), jnp.float32),
        pltpu.VMEM((members, rows, width), bf16),
        pltpu.VMEM((members, rows, width), bf16),
        pltpu.VMEM((reach_back + 1, pool_cols), bf16),
        pltpu.VMEM((reach_back + 1, pool_cols), bf16),
        pltpu.VMEM((rows, model), jnp.float32),
        pltpu.VMEM((half, model), bf16),
        dma((6,)),
        dma,
        dma((bands,)),
        dma((bands,)),
        dma((bands,)),
        dma((bands,)),
        dma((bands, members)),
        dma((bands, members)),
        dma((members,)),
        dma((members,)),
        dma((members,)),
        dma((members,)),
        dma,
        dma,
        dma,
        dma,
    ]


vmem_most = 67043328


def scratch_bytes(scratch):
    return sum(
        math.prod(item.shape) * jnp.dtype(item.dtype).itemsize
        for item in scratch
        if getattr(item, "memory_space", None) == pltpu.VMEM
    )


def whole_layer(
    normed,
    query_weight,
    key_weight,
    value_weight,
    pool_in_weight,
    pool_weight,
    map_balance,
    head_gain,
    contrast_out_weight,
    pool_out_weight,
):
    sp_count = lax.axis_size("sp")
    width = head_gain.shape[0]
    members = query_weight.shape[1] // width
    half, model = normed.shape
    pool_cols = pool_in_weight.shape[1]
    groups_here = pool_weight.shape[0]
    scratch = kernel_scratch(
        sp_count, max(members, 1), half, model, width, pool_cols
    )
    fits = (
        lax.axis_size("tp") == 2
        and members > 1
        and members & (members - 1) == 0
        and sp_count % members == 0
        and sp_count // members > 1
        and groups_here % 4 == 0
        and scratch_bytes(scratch) < vmem_most * 3 // 4
    )
    if not fits:
        return per_device(
            normed,
            query_weight,
            key_weight,
            value_weight,
            pool_in_weight,
            pool_weight,
            map_balance,
            head_gain,
            contrast_out_weight,
            pool_out_weight,
        )
    vmem = pl.BlockSpec(memory_space=pltpu.VMEM)
    hbm = pl.BlockSpec(memory_space=pl.ANY)
    own_part, partner_part = pl.pallas_call(
        functools.partial(layer_kernel, sp_count, members),
        out_shape=[jax.ShapeDtypeStruct((half, model), jnp.bfloat16)] * 2,
        in_specs=[vmem, vmem, pl.BlockSpec(memory_space=pltpu.SMEM), vmem] + [hbm] * 6,
        out_specs=[vmem, vmem],
        scratch_shapes=scratch,
        compiler_params=pltpu.CompilerParams(
            collective_id=0, has_side_effects=True, vmem_limit_bytes=vmem_most
        ),
    )(
        normed,
        pool_weight,
        map_balance,
        head_gain.reshape(1, width),
        query_weight,
        key_weight,
        value_weight,
        pool_in_weight,
        contrast_out_weight,
        pool_out_weight,
    )
    return (own_part.astype(jnp.float32) + partner_part.astype(jnp.float32)).astype(jnp.bfloat16)


def solution(mesh):
    return jax.shard_map(
        whole_layer,
        mesh=mesh,
        in_specs=(
            P(("sp", "tp"), None),
            P(None, "tp"),
            P(None, "tp"),
            P(None, "tp"),
            P(None, "tp"),
            P("tp", None, None),
            P(),
            P(),
            P("tp", None),
            P("tp", None),
        ),
        out_specs=P(("sp", "tp"), None),
        check_vma=False,
    )
```

```python
import functools
import math

import jax
import jax.numpy as jnp
from jax import lax
from jax.experimental import pallas as pl
from jax.experimental.pallas import tpu as pltpu
from jax.sharding import PartitionSpec as P

reach_back = 15
norm_epsilon = 1e-06


def passed_along(block, axis, distance):
    devices = range(lax.axis_size(axis))
    route = [(i - distance, i) for i in devices if i - distance in devices]
    return lax.ppermute(block, axis, route)


def from_partner(block, axis, stride):
    count = lax.axis_size(axis)
    route = []
    for low in range(count):
        high = low | 1 << stride
        if high != low and high < count:
            route += [(low, high), (high, low)]
    return lax.ppermute(block, axis, route)


def shifted(array, axis, by):
    size = lax.axis_size(axis)
    return lax.ppermute(array, axis, [(i, (i + by) % size) for i in range(size)])


def as_sent(array):

    def short(part):
        return part.astype(jnp.bfloat16) if part.dtype == jnp.float32 else part

    return jax.tree.map(short, array)


def attend(running, queries, key_rows, value_rows, query_first, key_first, score_scale):
    key_count = key_rows.shape[0]
    key_block = math.gcd(key_count, 1024)
    unit_count = queries.shape[1]
    heads_here = value_rows.shape[1]
    per_head = unit_count // heads_here
    query_count = queries.shape[0]
    query_order = query_first + lax.iota(jnp.int32, query_count)

    def key_step(block_index, carried):
        block_start = block_index * key_block

        def block_work(current):
            row_peak, row_total, weighted = current
            scores = (
                jnp.einsum("qud,kud->uqk", queries, key_rows, preferred_element_type=jnp.float32)
                * score_scale
            )
            key_order = key_first + block_start + lax.iota(jnp.int32, key_block)
            scores = jnp.where(
                key_order[None, None, :] <= query_order[None, :, None], scores, -jnp.inf
            )
            new_peak = jnp.maximum(row_peak, jnp.max(scores, axis=2))
            shrink = jnp.exp(row_peak - new_peak)
            raised = jnp.exp(scores - new_peak[:, :, None])
            row_total = row_total * shrink + jnp.sum(raised, axis=2)
            map_weights = raised.astype(jnp.bfloat16).reshape(
                heads_here, per_head, query_count, key_block
            )
            update = jnp.einsum(
                "hmqk,khe->hmqe", map_weights, value_rows, preferred_element_type=jnp.float32
            )
            weighted = weighted * shrink[:, :, None] + update.reshape(unit_count, query_count, -1)
            return (new_peak, row_total, weighted)

        def keep_state(current):
            return current

        return lax.cond(
            key_first + block_start <= query_first + query_count - 1,
            block_work,
            keep_state,
            carried,
        )

    return lax.fori_loop(0, key_count // key_block, key_step, running)


def fresh_state(unit_count, row_count, value_width):
    return (
        jnp.full((unit_count, row_count), -1e30, jnp.float32),
        jnp.zeros((unit_count, row_count), jnp.float32),
        jnp.zeros((unit_count, row_count, value_width), jnp.float32),
    )


def finished(running):
    row_peak, row_total, weighted = running
    return (weighted / row_total[:, :, None]).astype(jnp.bfloat16)


def joined_state(first, second):
    first_peak, first_total, first_weighted = first
    second_peak, second_total, second_weighted = second
    new_peak = jnp.maximum(first_peak, second_peak)
    first_shrink = jnp.exp(first_peak - new_peak)
    second_shrink = jnp.exp(second_peak - new_peak)
    new_total = first_total * first_shrink + second_total * second_shrink
    new_weighted = (
        first_weighted * first_shrink[:, :, None] + second_weighted * second_shrink[:, :, None]
    )
    return (new_peak, new_total, new_weighted)


def per_device(
    normed,
    query_weight,
    key_weight,
    value_weight,
    pool_in_weight,
    pool_weight,
    map_balance,
    head_gain,
    contrast_out_weight,
    pool_out_weight,
):
    tp_index = lax.axis_index("tp")
    sp_count = lax.axis_size("sp")
    sp_index = lax.axis_index("sp")
    head_dim = head_gain.shape[0] // 2
    value_width = 2 * head_dim
    query_cols = query_weight.shape[1]
    value_cols = value_weight.shape[1]
    unit_count = query_cols // head_dim
    heads_here = unit_count // 2
    project_incoming = lax.all_gather(normed, "tp", axis=0, tiled=True)
    products = [
        jnp.dot(project_incoming, weight_part, preferred_element_type=jnp.float32)
        for weight_part in (query_weight, key_weight, value_weight, pool_in_weight)
    ]
    joined = jnp.concatenate(products, axis=1).astype(jnp.bfloat16)
    row_count = joined.shape[0]
    queries = joined[:, :query_cols].reshape(row_count, unit_count, head_dim)
    key_rows = joined[:, query_cols : 2 * query_cols].reshape(row_count, unit_count, head_dim)
    value_rows = joined[:, 2 * query_cols : 2 * query_cols + value_cols].reshape(
        row_count, heads_here, value_width
    )
    pool_input = joined[:, 2 * query_cols + value_cols :]
    pool_cols = pool_input.shape[1]
    upper_rim = passed_along(pool_input[row_count - reach_back :], "sp", 1)
    extended = jnp.concatenate([upper_rim, pool_input], axis=0).astype(jnp.float32)
    groups_here = pool_weight.shape[0]
    group_width = pool_weight.shape[1]
    group_index = tp_index * groups_here + lax.iota(jnp.int32, pool_cols) // group_width
    widths = jnp.left_shift(jnp.int32(2), group_index % 4)
    window_sum = jnp.zeros((row_count, pool_cols), jnp.float32)
    for offset in range(reach_back + 1):
        window_sum = window_sum + extended[
            reach_back - offset : reach_back - offset + row_count
        ] * (offset < widths)[None, :].astype(jnp.float32)
    position = sp_index * row_count + lax.iota(jnp.int32, row_count)
    counts = jnp.minimum(position[:, None] + 1, widths[None, :]).astype(jnp.float32)
    spread = (window_sum / counts - extended[reach_back:]).astype(jnp.bfloat16)
    mixed_groups = jnp.einsum(
        "tgc,gce->tge",
        spread.reshape(row_count, groups_here, group_width),
        pool_weight,
        preferred_element_type=jnp.float32,
    )
    pool_out = mixed_groups.reshape(row_count, pool_cols).astype(jnp.bfloat16)
    score_scale = head_dim ** (-0.5)
    level_count = sp_count.bit_length() - 1
    low_levels = level_count // 2
    band_size = 1 << low_levels
    band_count = sp_count // band_size
    member = sp_index % band_size
    band = sp_index // band_size
    band_queries = queries
    for bit in range(low_levels):
        received = from_partner(band_queries, "sp", bit)
        upper = member >> bit & 1 == 1
        band_queries = jnp.where(
            upper,
            jnp.concatenate([received, band_queries], axis=0),
            jnp.concatenate([band_queries, received], axis=0),
        )
    band_first = band * band_size * row_count
    running = fresh_state(unit_count, band_size * row_count, value_width)
    for step in range(band_count):
        if step == 0:
            key_piece, value_piece = (key_rows, value_rows)
        else:
            key_piece, value_piece = shifted((key_rows, value_rows), "sp", step * band_size)
        source = (sp_index - step * band_size) % sp_count
        running = attend(
            running,
            band_queries,
            key_piece,
            value_piece,
            band_first,
            source * row_count,
            score_scale,
        )
    for bit in range(low_levels - 1, -1, -1):
        half = running[0].shape[1] // 2
        upper = member >> bit & 1 == 1
        lower_part = jax.tree.map(lambda item: item[:, :half], running)
        upper_part = jax.tree.map(lambda item: item[:, half:], running)
        outgoing = jax.tree.map(
            lambda low, high: jnp.where(upper, low, high), lower_part, upper_part
        )
        kept = jax.tree.map(lambda low, high: jnp.where(upper, high, low), lower_part, upper_part)
        incoming = from_partner(
            (as_sent(outgoing[0]), as_sent(outgoing[1]), as_sent(outgoing[2])), "sp", bit
        )
        running = joined_state(kept, incoming)
    maps = finished(running)
    paired = maps.reshape(heads_here, 2, row_count, value_width)
    paired = lax.optimization_barrier(paired).astype(jnp.float32)
    head_first = tp_index * heads_here
    balance_here = lax.dynamic_slice_in_dim(map_balance, head_first, heads_here, 0)
    contrast = paired[:, 0] - balance_here[:, None, None] * paired[:, 1]
    mean_square = jnp.mean(contrast * contrast, axis=2, keepdims=True)
    contrast = contrast * lax.rsqrt(mean_square + norm_epsilon) * head_gain
    contrast_out = (
        contrast.astype(jnp.bfloat16)
        .transpose(1, 0, 2)
        .reshape(row_count, heads_here * value_width)
    )
    partial_value = jnp.dot(contrast_out, contrast_out_weight, preferred_element_type=jnp.float32)
    return lax.psum_scatter(
        (
            partial_value + jnp.dot(pool_out, pool_out_weight, preferred_element_type=jnp.float32)
        ).astype(jnp.bfloat16),
        "tp",
        scatter_dimension=0,
        tiled=True,
    )


MESH = pl.DeviceIdType.MESH


def flipped(index, mask, size):
    total = 0
    bit = 1
    while bit < size:
        total = total + lax.rem(lax.div(index, bit) + lax.div(mask, bit), 2) * bit
        bit *= 2
    return total


def layer_kernel(
    sp_count,
    members,
    x_ref,
    pool_weight,
    balance,
    gain,
    query_hbm,
    key_hbm,
    value_hbm,
    pool_in_hbm,
    contrast_hbm,
    pool_out_hbm,
    out_ref,
    out_recv,
    query_w,
    key_w,
    value_w,
    pool_in_w,
    contrast_w,
    pool_out_w,
    rows_in,
    kv,
    kv_stage,
    queries,
    query_stage,
    peaks,
    totals,
    weighted,
    contrasts,
    contrast_stage,
    rim,
    rim_stage,
    pool_part,
    out_stage,
    weight_sem,
    local_sem,
    pair_send,
    pair_recv,
    relay_send,
    relay_recv,
    kv_send,
    kv_recv,
    query_send,
    query_recv,
    contrast_send,
    contrast_recv,
    rim_send,
    rim_recv,
    out_send,
    out_recv_sem,
):
    f32 = jnp.float32
    bf16 = jnp.bfloat16
    bands = sp_count // members
    sp = lax.axis_index("sp")
    tp = lax.axis_index("tp")
    other = 1 - tp
    band = lax.div(sp, members)
    member = lax.rem(sp, members)
    half, model = x_ref.shape
    rows = 2 * half
    width = gain.shape[1]
    head_dim = width // 2

    loads = [
        pltpu.make_async_copy(src, dst, weight_sem.at[i])
        for i, (src, dst) in enumerate(
            (
                (key_hbm, key_w),
                (value_hbm, value_w),
                (query_hbm, query_w),
                (pool_in_hbm, pool_in_w),
                (pool_out_hbm, pool_out_w),
                (contrast_hbm, contrast_w),
            )
        )
    ]
    for load in loads:
        load.start()
    keep = pltpu.make_async_copy(x_ref, rows_in.at[0, tp], local_sem)
    keep.start()

    barrier = pltpu.get_barrier_semaphore()
    greeted = [
        (sp, other),
        (lax.rem(sp + members, sp_count), tp),
        (lax.rem(sp + sp_count - members, sp_count), tp),
        (lax.rem(sp + 1, sp_count), tp),
        (lax.rem(sp + sp_count - 1, sp_count), tp),
    ]
    greeted += [(band * members + flipped(member, j, members), tp) for j in range(1, members)]
    for target in greeted:
        pl.semaphore_signal(barrier, inc=1, device_id=target, device_id_type=MESH)
    pl.semaphore_wait(barrier, len(greeted))

    def pair_copy(step):
        return pltpu.make_async_remote_copy(
            src_ref=x_ref if step == 0 else rows_in.at[step, tp],
            dst_ref=rows_in.at[step, tp],
            send_sem=pair_send.at[step],
            recv_sem=pair_recv.at[step],
            device_id=(sp, other),
            device_id_type=MESH,
        )

    def relay_copy(step):
        return pltpu.make_async_remote_copy(
            src_ref=x_ref if step == 1 else rows_in.at[step - 1, tp],
            dst_ref=rows_in.at[step, tp],
            send_sem=relay_send.at[step],
            recv_sem=relay_recv.at[step],
            device_id=(lax.rem(sp + members, sp_count), tp),
            device_id_type=MESH,
        )

    def kv_copy(step, j):
        return pltpu.make_async_remote_copy(
            src_ref=kv_stage.at[step, j],
            dst_ref=kv.at[step, member],
            send_sem=kv_send.at[step, j],
            recv_sem=kv_recv.at[step, j],
            device_id=(band * members + flipped(member, j, members), tp),
            device_id_type=MESH,
        )

    def query_copy(j):
        return pltpu.make_async_remote_copy(
            src_ref=query_stage.at[j],
            dst_ref=queries.at[member],
            send_sem=query_send.at[j],
            recv_sem=query_recv.at[j],
            device_id=(band * members + flipped(member, j, members), tp),
            device_id_type=MESH,
        )

    def contrast_copy(j):
        return pltpu.make_async_remote_copy(
            src_ref=contrast_stage.at[j],
            dst_ref=contrasts.at[member],
            send_sem=contrast_send.at[j],
            recv_sem=contrast_recv.at[j],
            device_id=(band * members + flipped(member, j, members), tp),
            device_id_type=MESH,
        )

    rim_copy = pltpu.make_async_remote_copy(
        src_ref=rim_stage,
        dst_ref=rim,
        send_sem=rim_send,
        recv_sem=rim_recv,
        device_id=(lax.rem(sp + 1, sp_count), tp),
        device_id_type=MESH,
    )
    out_copy = pltpu.make_async_remote_copy(
        src_ref=out_stage,
        dst_ref=out_recv,
        send_sem=out_send,
        recv_sem=out_recv_sem,
        device_id=(sp, other),
        device_id_type=MESH,
    )

    pair_copy(0).start()

    @pl.when(band + 1 < bands)
    def _():
        relay_copy(1).start()

    def project(step):
        def one(t, carry):
            j = lax.rem(t + 1, members)
            head = flipped(member, j, members)
            columns = pl.ds(pl.multiple_of(head * width, width), width)
            x = rows_in[step].reshape(rows, model)
            keys = jnp.dot(x, key_w[:, columns], preferred_element_type=f32).astype(bf16)
            values = jnp.dot(x, value_w[:, columns], preferred_element_type=f32).astype(bf16)

            @pl.when(j > 0)
            def _():
                kv_stage[step, j, :, :width] = keys
                kv_stage[step, j, :, width:] = values
                kv_copy(step, j).start()

            @pl.when(j == 0)
            def _():
                kv[step, member, :, :width] = keys
                kv[step, member, :, width:] = values

            if step == 0:
                mine = jnp.dot(x, query_w[:, columns], preferred_element_type=f32).astype(bf16)

                @pl.when(j > 0)
                def _():
                    query_stage[j] = mine
                    query_copy(j).start()

                @pl.when(j == 0)
                def _():
                    queries[member] = mine

            return carry

        lax.fori_loop(0, members, one, 0)

    def take_band(step):
        @pl.when(band >= step)
        def _():
            relay_copy(step).wait_recv()
            if step + 1 < bands:

                @pl.when(band + 1 < bands)
                def _():
                    relay_copy(step + 1).start()

            pair_copy(step).start()
            pair_copy(step).wait_recv()
            project(step)

    log_scale = head_dim ** (-0.5) * math.log2(math.e)

    def attend_block(step, i, blocks):
        seen = len(blocks)
        for u in range(2):
            cols = slice(u * head_dim, (u + 1) * head_dim)
            keys = jnp.concatenate([kv[step, b, :, cols] for b in blocks], axis=0)
            values = jnp.concatenate([kv[step, b, :, width:] for b in blocks], axis=0)
            scores = lax.dot_general(
                queries[i, :, cols], keys, (((1,), (1,)), ((), ())), preferred_element_type=f32
            )
            if step == 0:
                query_order = lax.broadcasted_iota(jnp.int32, scores.shape, 0) + (seen - 1) * rows
                key_order = lax.broadcasted_iota(jnp.int32, scores.shape, 1)
                scores = jnp.where(key_order <= query_order, scores, -jnp.inf)
            peak = jnp.max(scores, axis=1, keepdims=True)
            if step > 0:
                old = peaks[u, i][:, :1]
                peak = jnp.maximum(peak, old)
                shrink = jnp.exp2((old - peak) * log_scale)
            raised = jnp.exp2((scores - peak) * log_scale)
            total = jnp.sum(raised, axis=1, keepdims=True)
            update = jnp.dot(raised.astype(bf16), values, preferred_element_type=f32)
            if step > 0:
                total = total + totals[u, i][:, :1] * shrink
                update = update + weighted[u, i] * shrink
            peaks[u, i] = jnp.broadcast_to(peak, peaks.shape[2:])
            totals[u, i] = jnp.broadcast_to(total, totals.shape[2:])
            weighted[u, i] = update

    weight = balance[tp * members + member]

    def finish(i, j):
        first = (weighted[0, i] / totals[0, i][:, :1]).astype(bf16).astype(f32)
        second = (weighted[1, i] / totals[1, i][:, :1]).astype(bf16).astype(f32)
        contrast = first - weight * second
        mean_square = jnp.mean(contrast * contrast, axis=1, keepdims=True)
        result = (contrast * lax.rsqrt(mean_square + norm_epsilon) * gain[...]).astype(bf16)

        @pl.when(j > 0)
        def _():
            contrast_stage[j] = result
            contrast_copy(j).start()

        @pl.when(j == 0)
        def _():
            contrasts[member] = result

    def attend_own():
        for j in range(1, members):
            query_copy(j).wait_recv()
            kv_copy(0, j).wait_recv()
        for i in range(members):
            attend_block(0, i, list(range(i + 1)))

            @pl.when(band == 0)
            def _(i=i):
                finish(i, flipped(member, i, members))

    parts = (list(range(members)),)

    def attend_band(step):
        @pl.when(band >= step)
        def _():
            for part in parts:
                for j in part:
                    if j > 0:
                        kv_copy(step, j).wait_recv()
                blocks = [flipped(member, j, members) for j in part]

                def one(t, carry, part=part, blocks=blocks):
                    j = lax.rem(t + 1, members)
                    i = flipped(member, j, members)
                    attend_block(step, i, blocks)
                    if part is parts[-1]:

                        @pl.when(band == step)
                        def _():
                            finish(i, j)

                    return carry

                lax.fori_loop(0, members, one, 0)

    keep.wait()
    loads[0].wait()
    loads[1].wait()
    loads[2].wait()
    pair_copy(0).wait_recv()
    project(0)

    loads[3].wait()
    pool_input = jnp.dot(
        rows_in[0].reshape(rows, model), pool_in_w[...], preferred_element_type=f32
    ).astype(bf16)
    rim_stage[...] = pool_input[rows - rim.shape[0] :]

    @pl.when(sp + 1 < sp_count)
    def _():
        rim_copy.start()

    take_band(1)

    @pl.when(sp > 0)
    def _():
        rim_copy.wait_recv()

    @pl.when(sp == 0)
    def _():
        rim[...] = jnp.zeros_like(rim)

    loads[4].wait()
    extended = jnp.concatenate([rim[...], pool_input], axis=0).astype(f32)
    group_width = pool_weight.shape[1]
    skirt = rim.shape[0]
    position = sp * rows + lax.broadcasted_iota(jnp.int32, (rows, group_width), 0)
    mixed = []
    for group in range(pool_weight.shape[0]):
        block = extended[:, group * group_width : (group + 1) * group_width]
        window = block
        reach = 1
        span = 2 ** (1 + group % 4)
        while reach < span:
            window = window + pltpu.roll(window, reach, 0)
            reach *= 2
        counts = jnp.minimum(position + 1, span).astype(f32)
        spread = (window[skirt:] / counts - block[skirt:]).astype(bf16)
        mixed.append(
            jnp.dot(spread, pool_weight[group], preferred_element_type=f32).astype(bf16)
        )
    pool_out = jnp.concatenate(mixed, axis=1)
    chunk = math.gcd(model, 512)
    for start in range(0, model, chunk):
        pool_part[:, start : start + chunk] = jnp.dot(
            pool_out, pool_out_w[:, start : start + chunk], preferred_element_type=f32
        )

    for step in range(2, bands):
        take_band(step)
        if step == 2:
            attend_own()
        else:
            attend_band(step - 2)
    if bands == 2:
        attend_own()
    for step in range(max(bands - 2, 1), bands):
        attend_band(step)

    loads[5].wait()
    for j in range(1, members):
        contrast_copy(j).wait_recv()

    def projected(side, store):
        taken = pl.ds(pl.multiple_of(side * half, half), half)
        left = jnp.concatenate([contrasts[h, taken, :] for h in range(members)], axis=1)
        for start in range(0, model, chunk):
            cut = slice(start, start + chunk)
            part = jnp.dot(left, contrast_w[:, cut], preferred_element_type=f32)
            store(cut, (part + pool_part[taken, cut]).astype(bf16))

    def to_partner(cut, part):
        out_stage[:, cut] = part

    def to_self(cut, part):
        out_ref[:, cut] = part

    projected(other, to_partner)
    out_copy.start()
    projected(tp, to_self)
    out_copy.wait()
    pair_copy(0).wait_send()
    for j in range(1, members):
        query_copy(j).wait_send()
        kv_copy(0, j).wait_send()
        contrast_copy(j).wait_send()

    @pl.when(sp + 1 < sp_count)
    def _():
        rim_copy.wait_send()

    for step in range(1, bands):

        @pl.when(jnp.logical_and(band + 1 < bands, band >= step - 1))
        def _(step=step):
            relay_copy(step).wait_send()

        @pl.when(band >= step)
        def _(step=step):
            pair_copy(step).wait_send()
            for j in range(1, members):
                kv_copy(step, j).wait_send()


def kernel_scratch(sp_count, members, half, model, width, pool_cols):
    bf16 = jnp.bfloat16
    bands = sp_count // members
    rows = 2 * half
    columns = members * width
    dma = pltpu.SemaphoreType.DMA
    return [
        pltpu.VMEM((model, columns), bf16),
        pltpu.VMEM((model, columns), bf16),
        pltpu.VMEM((model, columns), bf16),
        pltpu.VMEM((model, pool_cols), bf16),
        pltpu.VMEM((columns, model), bf16),
        pltpu.VMEM((pool_cols, model), bf16),
        pltpu.VMEM((bands, 2, half, model), bf16),
        pltpu.VMEM((bands, members, rows, 2 * width), bf16),
        pltpu.VMEM((bands, members, rows, 2 * width), bf16),
        pltpu.VMEM((members, rows, width), bf16),
        pltpu.VMEM((members, rows, width), bf16),
        pltpu.VMEM((2, members, rows, 128), jnp.float32),
        pltpu.VMEM((2, members, rows, 128), jnp.float32),
        pltpu.VMEM((2, members, rows, width), jnp.float32),
        pltpu.VMEM((members, rows, width), bf16),
        pltpu.VMEM((members, rows, width), bf16),
        pltpu.VMEM((reach_back + 1, pool_cols), bf16),
        pltpu.VMEM((reach_back + 1, pool_cols), bf16),
        pltpu.VMEM((rows, model), jnp.float32),
        pltpu.VMEM((half, model), bf16),
        dma((6,)),
        dma,
        dma((bands,)),
        dma((bands,)),
        dma((bands,)),
        dma((bands,)),
        dma((bands, members)),
        dma((bands, members)),
        dma((members,)),
        dma((members,)),
        dma((members,)),
        dma((members,)),
        dma,
        dma,
        dma,
        dma,
    ]


vmem_most = 67043328


def scratch_bytes(scratch):
    return sum(
        math.prod(item.shape) * jnp.dtype(item.dtype).itemsize
        for item in scratch
        if getattr(item, "memory_space", None) == pltpu.VMEM
    )


def whole_layer(
    normed,
    query_weight,
    key_weight,
    value_weight,
    pool_in_weight,
    pool_weight,
    map_balance,
    head_gain,
    contrast_out_weight,
    pool_out_weight,
):
    sp_count = lax.axis_size("sp")
    width = head_gain.shape[0]
    members = query_weight.shape[1] // width
    half, model = normed.shape
    pool_cols = pool_in_weight.shape[1]
    groups_here = pool_weight.shape[0]
    scratch = kernel_scratch(
        sp_count, max(members, 1), half, model, width, pool_cols
    )
    fits = (
        lax.axis_size("tp") == 2
        and members > 1
        and members & (members - 1) == 0
        and sp_count % members == 0
        and sp_count // members > 1
        and groups_here % 4 == 0
        and scratch_bytes(scratch) < vmem_most * 3 // 4
    )
    if not fits:
        return per_device(
            normed,
            query_weight,
            key_weight,
            value_weight,
            pool_in_weight,
            pool_weight,
            map_balance,
            head_gain,
            contrast_out_weight,
            pool_out_weight,
        )
    vmem = pl.BlockSpec(memory_space=pltpu.VMEM)
    hbm = pl.BlockSpec(memory_space=pl.ANY)
    own_part, partner_part = pl.pallas_call(
        functools.partial(layer_kernel, sp_count, members),
        out_shape=[jax.ShapeDtypeStruct((half, model), jnp.bfloat16)] * 2,
        in_specs=[vmem, vmem, pl.BlockSpec(memory_space=pltpu.SMEM), vmem] + [hbm] * 6,
        out_specs=[vmem, vmem],
        scratch_shapes=scratch,
        compiler_params=pltpu.CompilerParams(
            collective_id=0, has_side_effects=True, vmem_limit_bytes=vmem_most
        ),
    )(
        normed,
        pool_weight,
        map_balance,
        head_gain.reshape(1, width),
        query_weight,
        key_weight,
        value_weight,
        pool_in_weight,
        contrast_out_weight,
        pool_out_weight,
    )
    return (own_part.astype(jnp.float32) + partner_part.astype(jnp.float32)).astype(jnp.bfloat16)


def solution(mesh):
    return jax.shard_map(
        whole_layer,
        mesh=mesh,
        in_specs=(
            P(("sp", "tp"), None),
            P(None, "tp"),
            P(None, "tp"),
            P(None, "tp"),
            P(None, "tp"),
            P("tp", None, None),
            P(),
            P(),
            P("tp", None),
            P("tp", None),
        ),
        out_specs=P(("sp", "tp"), None),
        check_vma=False,
    )
```
